32 devices in a mesh: sp: 8 (over z, y), tp: 4 (over x, core).
Axes of the slice: x: 2, y: 2, z: 4, core: 2. Of those that a mesh axis runs over, the one named last changes fastest.
Arguments:
- tokens: bfloat16 [1536, 2048], P('sp'), may hold values from -6 to 6
- norm_gain: float32 [2048], replicated, may hold values from 0.1 to 1.9
- conv_value_w: bfloat16 [2048, 1024], P('sp', 'tp'), may hold values from -0.125 to 0.125
- conv_gate_w: bfloat16 [2048, 1024], P('sp', 'tp'), may hold values from -0.125 to 0.125
- query_w: bfloat16 [2048, 1024], P('sp', 'tp'), may hold values from -0.125 to 0.125
- key_w: bfloat16 [2048, 1024], P('sp', 'tp'), may hold values from -0.125 to 0.125
- value_w: bfloat16 [2048, 1024], P('sp', 'tp'), may hold values from -0.125 to 0.125
- out_gate_w: bfloat16 [2048, 1024], P('sp', 'tp'), may hold values from -0.125 to 0.125
- conv_out_w: bfloat16 [2048, 1024], P('sp', 'tp'), may hold values from -0.125 to 0.125
- ret_out_w: bfloat16 [2048, 1024], P('sp', 'tp'), may hold values from -0.125 to 0.125
- conv_taps: bfloat16 [31, 1024], replicated, may hold values from -3 to 3
- conv_gain: float32 [1024], replicated, may hold values from 0.1 to 1.9
- ret_gain: float32 [1024], replicated, may hold values from 0.1 to 1.9
- log_decay: float32 [8, 1536], P('tp', 'sp'), may hold values from -1 to 0, as said below
Outputs:
- mixed: bfloat16 [1536, 2048], P(('sp', 'tp'))
The draws below stay inside these ranges and needn't reach their ends.
Inputs may be any that keep to these rules, and one draw needn't show every extreme that they name: `log_decay`: every entry is at most zero.
All inputs are finite; a program needn't handle non-finite values.
Results may differ from the reference program's by a relative error of at most 0.03.
Values may be sent and summed in bfloat16 or wider, within the bound.
A program may use at most 64 MiB of HBM per device.

```python
import math
import jax
import jax.numpy as jnp
from jax import lax

D = 2048
CONV_DIM = 1024
RET_HEADS = 8
HEAD_DIM = 128
CONV_WIDTH = 31
TOK_DEV = 192
RET_DIM = 1024
TOKEN_COUNT = 1536
N_SP = 8
N_TP = 4


def draw_log_decay(key, part):
    base_key = jax.random.fold_in(key, 17)
    order_key, fast_key, block_key, location_random_key, depth_key = jax.random.split(base_key, 5)
    ranking = jax.random.permutation(order_key, RET_HEADS)
    fast_head = ranking < RET_HEADS // 2
    fast_rate = -1.0 / jax.random.uniform(fast_key, (RET_HEADS,), jnp.float32, 30.0, 50.0)
    slow_rate = jnp.full((RET_HEADS,), -math.log(10.0) / (4.0 * TOKEN_COUNT), jnp.float32)
    head_decay_rate = jnp.where(fast_head, fast_rate, slow_rate)
    block_factor = jnp.exp(jax.random.uniform(block_key, (TOKEN_COUNT // TOK_DEV,), jnp.float32, -math.log(2.0), math.log(2.0)))
    position_scale_factor = jnp.repeat(block_factor, TOK_DEV, total_repeat_length=TOKEN_COUNT)
    spike_locations = jax.random.randint(location_random_key, (3,), 0, TOKEN_COUNT)
    layer_depths = jnp.log(jax.random.uniform(depth_key, (3,), jnp.float32, 0.5, 0.8))
    token_positions = jnp.arange(TOKEN_COUNT, dtype=jnp.int32)
    spike_values = jnp.sum(jnp.where(token_positions[:, None] == spike_locations[None, :], layer_depths[None, :], 0.0), axis=1)
    return (head_decay_rate[:, None] * position_scale_factor[None, :] + spike_values[None, :]).astype(jnp.float32)


def draw_conv_taps(key, part):
    base_key = jax.random.fold_in(key, 29)
    tap_noise = jnp.clip(jax.random.normal(base_key, (CONV_WIDTH, CONV_DIM), jnp.float32), -4.0, 4.0)
    rise_ratio = 5.0
    channel = jnp.arange(CONV_DIM, dtype=jnp.float32) / (CONV_DIM - 1)
    chan_scale = jnp.exp(math.log(rise_ratio) * (channel - 0.5))
    return (tap_noise * chan_scale[None, :] / math.sqrt(CONV_WIDTH)).astype(jnp.bfloat16)


def steps_of(key, dims, cuts, smallest, largest):
    factor_of = 1.0
    for dim, parts in cuts:
        steps = jax.random.uniform(jax.random.fold_in(jax.random.fold_in(key, 6), dim), (parts,), jnp.float32, smallest / len(cuts), largest / len(cuts))
        factor_of = factor_of * jnp.repeat(jnp.exp(steps), dims[dim] // parts).reshape((-1,) + (1,) * (len(dims) - 1 - dim))
    return factor_of


def gaussian(key, shape, deviation, reach, pieces=(), held_as=jnp.bfloat16):
    loudness = steps_of(key, shape, pieces, -0.22, 0.18) if pieces else 1.0
    entries = jax.random.normal(key, shape, jnp.float32) * deviation * loudness
    return jnp.minimum(jnp.maximum(entries, -reach), reach).astype(held_as)


def setup_inputs(seed: int = 0) -> dict:
    splits = jax.random.split(jax.random.key(seed), 15)
    return {
        "tokens": gaussian(splits[0], (TOKEN_COUNT, D), 1.0, 6.0, ((0, 8),)),
        "norm_gain": jnp.clip(1.0 + 0.18 * jax.random.normal(splits[1], (D,), jnp.float32), 0.1, 1.9),
        "conv_value_w": gaussian(splits[2], (D, CONV_DIM), D ** -0.5, 0.125, ((0, 8), (1, 4))),
        "conv_gate_w": gaussian(splits[3], (D, CONV_DIM), D ** -0.5, 0.125, ((0, 8), (1, 4))),
        "query_w": gaussian(splits[4], (D, RET_DIM), D ** -0.5, 0.125, ((0, 8), (1, 4))),
        "key_w": gaussian(splits[5], (D, RET_DIM), D ** -0.5, 0.125, ((0, 8), (1, 4))),
        "value_w": gaussian(splits[6], (D, RET_DIM), D ** -0.5, 0.125, ((0, 8), (1, 4))),
        "out_gate_w": gaussian(splits[7], (D, RET_DIM), D ** -0.5, 0.125, ((0, 8), (1, 4))),
        "conv_out_w": gaussian(splits[8], (D, CONV_DIM), (CONV_DIM + RET_DIM) ** -0.5, 0.125, ((0, 8), (1, 4))),
        "ret_out_w": gaussian(splits[9], (D, RET_DIM), (CONV_DIM + RET_DIM) ** -0.5, 0.125, ((0, 8), (1, 4))),
        "conv_taps": draw_conv_taps(jax.random.fold_in(splits[14], 71), 0),
        "conv_gain": jnp.clip(1.0 + 0.18 * jax.random.normal(splits[11], (CONV_DIM,), jnp.float32), 0.1, 1.9),
        "ret_gain": jnp.clip(1.0 + 0.18 * jax.random.normal(splits[12], (RET_DIM,), jnp.float32), 0.1, 1.9),
        "log_decay": draw_log_decay(jax.random.fold_in(splits[14], 71), 0),
    }


EPSILON = 1e-06
ROPE_BASE = 10000.0

def rotate(values, token_positions):
    half_dim = values.shape[-1] // 2
    frequency = ROPE_BASE ** (-jnp.arange(0, 2 * half_dim, 2, dtype=jnp.float32) / (2 * half_dim))
    angles = token_positions.astype(jnp.float32)[:, None] * frequency[None, :]
    cosine = jnp.cos(angles)[:, None, :]
    sine_part = jnp.sin(angles)[:, None, :]
    first_half = values[..., :half_dim]
    second = values[..., half_dim:]
    return jnp.concatenate([first_half * cosine - second * sine_part, first_half * sine_part + second * cosine], axis=-1)

def reference(tokens, norm_gain, conv_value_w, conv_gate_w, query_w, key_w, value_w, out_gate_w, conv_out_w, ret_out_w, conv_taps, conv_gain, ret_gain, log_decay):
    block_tokens = tokens.reshape(N_SP, TOK_DEV, D)
    block_decay = jnp.transpose(log_decay.reshape(RET_HEADS, N_SP, TOK_DEV), (1, 0, 2))
    block_index = jnp.arange(N_SP, dtype=jnp.int32)
    taps_float = conv_taps.astype(jnp.float32)
    conv_group = CONV_DIM // N_TP
    ret_group = RET_DIM // N_TP
    conv_out_float = conv_out_w.astype(jnp.float32).reshape(D, N_TP, conv_group)
    ret_out_float = ret_out_w.astype(jnp.float32).reshape(D, N_TP, ret_group)
    token_iota = jnp.arange(TOK_DEV, dtype=jnp.int32)
    later_mask = token_iota[:, None] >= token_iota[None, :]

    def one_block(carry, inputs):
        state, rim_rows = carry
        x_block, decay_block, index = inputs
        tok_float = x_block.astype(jnp.float32)
        normed = (tok_float * lax.rsqrt(lax.optimization_barrier(jnp.mean(tok_float * tok_float, axis=-1, keepdims=True)) + EPSILON) * norm_gain).astype(jnp.bfloat16)

        def project(weight):
            return jnp.dot(normed, weight, preferred_element_type=jnp.float32).astype(jnp.bfloat16)
        conv_value = project(conv_value_w)
        conv_gate = project(conv_gate_w)
        conv_gated = (conv_value.astype(jnp.float32) * jax.nn.sigmoid(conv_gate.astype(jnp.float32))).astype(jnp.bfloat16)
        padded = jnp.concatenate([rim_rows, conv_gated], axis=0)
        conv_sum = jnp.zeros((TOK_DEV, CONV_DIM), jnp.float32)
        for tap_index in range(CONV_WIDTH):
            conv_sum = conv_sum + padded[tap_index:tap_index + TOK_DEV].astype(jnp.float32) * taps_float[tap_index]
        chan_mean = lax.optimization_barrier(jnp.sum(conv_sum, axis=-1, keepdims=True)) / CONV_DIM
        chan_square = lax.optimization_barrier(jnp.sum(conv_sum * conv_sum, axis=-1, keepdims=True)) / CONV_DIM
        chan_var = chan_square - chan_mean * chan_mean
        conv_hidden = jax.nn.silu((conv_sum - chan_mean) * lax.rsqrt(chan_var + EPSILON) * conv_gain).astype(jnp.bfloat16)
        token_positions = index * TOK_DEV + token_iota
        query_rows = (rotate(project(query_w).astype(jnp.float32).reshape(TOK_DEV, RET_HEADS, HEAD_DIM), token_positions) * HEAD_DIM ** (-0.5)).astype(jnp.bfloat16)
        key_rows = rotate(project(key_w).astype(jnp.float32).reshape(TOK_DEV, RET_HEADS, HEAD_DIM), token_positions).astype(jnp.bfloat16)
        value_rows = project(value_w).reshape(TOK_DEV, RET_HEADS, HEAD_DIM)
        out_gate = project(out_gate_w)
        running = jnp.cumsum(decay_block, axis=1)
        log_gap = running[:, :, None] - running[:, None, :]
        decay_matrix = jnp.where(later_mask[None], jnp.exp(jnp.where(later_mask[None], log_gap, 0.0)), 0.0)
        scores = jnp.einsum('thd,shd->hts', query_rows.astype(jnp.float32), key_rows.astype(jnp.float32))
        weights_intra = (scores * decay_matrix).astype(jnp.bfloat16)
        intra_part = jnp.einsum('hts,shd->thd', weights_intra.astype(jnp.float32), value_rows.astype(jnp.float32))
        to_end = jnp.exp(running[:, -1:] - running)
        key_weighted = (key_rows.astype(jnp.float32) * jnp.transpose(to_end)[:, :, None]).astype(jnp.bfloat16)
        block_state = jnp.einsum('thd,the->hde', key_weighted.astype(jnp.float32), value_rows.astype(jnp.float32))
        cross_part = jnp.einsum('thd,hde->the', query_rows.astype(jnp.float32), state, precision=lax.Precision.HIGHEST) * jnp.transpose(jnp.exp(running))[:, :, None]
        merged = intra_part + cross_part
        new_state = state * jnp.exp(running[:, -1])[:, None, None] + block_state
        head_mean = lax.optimization_barrier(jnp.mean(merged, axis=-1, keepdims=True))
        head_var = lax.optimization_barrier(jnp.mean(jnp.square(merged - head_mean), axis=-1, keepdims=True))
        ret_norm = ((merged - head_mean) * lax.rsqrt(head_var + EPSILON)).reshape(TOK_DEV, RET_DIM) * ret_gain
        ret_hidden = (jax.nn.silu(out_gate.astype(jnp.float32)) * ret_norm).astype(jnp.bfloat16)
        conv_part = jnp.einsum('tgc,dgc->gtd', conv_hidden.astype(jnp.float32).reshape(TOK_DEV, N_TP, conv_group), conv_out_float)
        ret_part = jnp.einsum('tgc,dgc->gtd', ret_hidden.astype(jnp.float32).reshape(TOK_DEV, N_TP, ret_group), ret_out_float)
        partial_value = (conv_part + ret_part).astype(jnp.bfloat16)
        mixed = lax.optimization_barrier(jnp.sum(partial_value.astype(jnp.float32), axis=0)).astype(jnp.bfloat16)
        return ((new_state, conv_gated[TOK_DEV - CONV_WIDTH + 1:]), mixed)
    start_state = jnp.zeros((RET_HEADS, HEAD_DIM, HEAD_DIM), jnp.float32)
    start_rim = jnp.zeros((CONV_WIDTH - 1, CONV_DIM), jnp.bfloat16)
    final_carry, outputs = lax.scan(one_block, (start_state, start_rim), (block_tokens, block_decay, block_index))
    return outputs.reshape(TOKEN_COUNT, D)
```

```python
import functools

import jax
import jax.numpy as jnp
import numpy as np
from jax import lax
from jax.experimental import pallas as pl
from jax.experimental.pallas import tpu as pltpu
from jax.sharding import PartitionSpec as P

HEAD_DIM = 128
EPSILON = 1e-06
ROPE_BASE = 10000.0
F32 = jnp.float32
BF16 = jnp.bfloat16
N_PROJ = 6
HALO = 32
CHUNKS = 4


def dot(a, b, ca=1, cb=0):
    return lax.dot_general(a, b, (((ca,), (cb,)), ((), ())), preferred_element_type=F32)


def kernel(
    n_s,
    n_t,
    conv_dim,
    tok_ref,
    gain_ref,
    kw_ref,
    vw_ref,
    cvw_ref,
    cgw_ref,
    qw_ref,
    ogw_ref,
    cow_ref,
    row_ref,
    taps_ref,
    cgain_ref,
    rgain_ref,
    ld_ref,
    cj_ref,
    sj_ref,
    cb_ref,
    sb_ref,
    out_ref,
    tok,
    x_self,
    x_send,
    x_recv,
    wbuf,
    obuf,
    acc,
    p_send,
    p_recv,
    decay,
    run_cols,
    tot_send,
    tot_buf,
    st_send,
    st_buf,
    state,
    halo_send,
    halo_recv,
    xp,
    csum,
    stat_send,
    stat_buf,
    hid,
    r_send,
    r_buf,
    qkv,
    loc_sem,
    x_sem,
    ws_sem,
    wr_sem,
    os_sem,
    or_sem,
    oy_sem,
    p_sem,
    ts_sem,
    tr_sem,
    ss_sem,
    sr_sem,
    h_sem,
    stat_sem,
    rs_sem,
):
    rows = tok.shape[0]
    wrows, cols = kw_ref.shape
    heads = cols // HEAD_DIM
    k = max(1, 128 // wrows)
    n_o = n_s // 2
    me = lax.axis_index("sp")
    mt = lax.axis_index("tp")
    half = lax.rem(me // k, 2)
    idx = (me // (2 * k)) * k + lax.rem(me, k)
    pair = me + k * (1 - 2 * half)

    def member(i):
        return (i // k) * (2 * k) + half * k + lax.rem(i, k)

    def remote(src, dst, ssem, rsem, where):
        return pltpu.make_async_remote_copy(
            src_ref=src,
            dst_ref=dst,
            send_sem=ssem,
            recv_sem=rsem,
            device_id=where,
            device_id_type=pl.DeviceIdType.MESH,
        )

    proj_refs = (kw_ref, vw_ref, cvw_ref, cgw_ref, qw_ref, ogw_ref)
    out_refs = (cow_ref, row_ref)

    tok_copy = pltpu.make_async_copy(tok_ref, tok, loc_sem.at[0])
    tok_copy.start()
    barrier = pltpu.get_barrier_semaphore()

    def greet_sp(d, c):
        pl.semaphore_signal(
            barrier,
            inc=1,
            device_id={"sp": lax.rem(me + d, n_s)},
            device_id_type=pl.DeviceIdType.MESH,
        )
        return c

    def greet_tp(d, c):
        pl.semaphore_signal(
            barrier,
            inc=1,
            device_id={"tp": lax.rem(mt + d, n_t)},
            device_id_type=pl.DeviceIdType.MESH,
        )
        return c

    lax.fori_loop(1, n_s, greet_sp, 0)
    lax.fori_loop(1, n_t, greet_tp, 0)

    def wslot(b, m):
        return wbuf.at[m, pl.ds(pl.multiple_of(b * wrows, wrows), wrows)]

    def oslot(s, m):
        return obuf.at[m, pl.ds(pl.multiple_of(s * wrows, wrows), wrows)]

    local = [
        pltpu.make_async_copy(r, wslot(idx, m), loc_sem.at[1 + m]) for m, r in enumerate(proj_refs)
    ] + [
        pltpu.make_async_copy(r, oslot(me, m), loc_sem.at[1 + N_PROJ + m])
        for m, r in enumerate(out_refs)
    ]
    for copy in local:
        copy.start()

    pl.semaphore_wait(barrier, n_s - 1 + n_t - 1)

    has_right = idx + 1 < n_o
    has_left = idx >= 1
    right = member(jnp.minimum(idx + 1, n_o - 1))
    left = member(jnp.maximum(idx - 1, 0))

    def w_copy(direction, b, m, src=None):
        slot = wslot(b, m)
        return remote(
            slot if src is None else src,
            slot,
            ws_sem.at[direction, b, m],
            wr_sem.at[direction, b, m],
            {"sp": right if direction == 0 else left},
        )

    @pl.when(has_right)
    def _():
        for m in range(N_PROJ):
            w_copy(0, idx, m, proj_refs[m]).start()

    @pl.when(has_left)
    def _():
        for m in range(N_PROJ):
            w_copy(1, idx, m, proj_refs[m]).start()

    tok_copy.wait()
    step = 256
    square = jnp.zeros((rows, 1), F32)
    for c in range(0, tok.shape[1], step):
        part = tok[:, c : c + step].astype(F32)
        square = square + jnp.sum(part * part, axis=1, keepdims=True)
    scale = lax.rsqrt(square / tok.shape[1] + EPSILON)
    width = k * wrows
    for j in range(n_s // (2 * k)):
        for side, dst in ((1 - half, x_send), (half, x_self)):
            start = pl.multiple_of((2 * j + side) * width, 128)
            part = tok[:, pl.ds(start, width)].astype(F32)
            dst[:, j * width : (j + 1) * width] = (
                part * scale * gain_ref[:, pl.ds(start, width)]
            ).astype(BF16)
    x_copy = remote(x_send, x_recv, x_sem.at[0], x_sem.at[1], {"sp": pair})
    x_copy.start()

    tot_send[...] = jnp.zeros_like(tot_send)
    r_iota = lax.broadcasted_iota(jnp.int32, (rows, rows), 0)
    c_iota = lax.broadcasted_iota(jnp.int32, (rows, rows), 1)
    for h in range(heads):
        ld = ld_ref[h : h + 1, :]
        ld_col = jnp.sum(jnp.where(r_iota == c_iota, ld, 0.0), axis=1, keepdims=True)
        run_col = jnp.sum(jnp.where(c_iota <= r_iota, ld, 0.0), axis=1, keepdims=True)
        run_row = jnp.sum(jnp.where(r_iota <= c_iota, ld_col, 0.0), axis=0, keepdims=True)
        keep = c_iota <= r_iota
        decay[h] = jnp.where(keep, jnp.exp(jnp.where(keep, run_col - run_row, 0.0)), 0.0)
        run_cols[h] = jnp.broadcast_to(run_col, (rows, HEAD_DIM))
        tot_send[h : h + 1, :] = jnp.broadcast_to(run_col[rows - 1 : rows], (1, HEAD_DIM))

    def tot_copy(to, source):
        return remote(
            tot_send, tot_buf.at[source], ts_sem.at[to], tr_sem.at[source], {"sp": to}
        )

    def start_tot(to, c):
        tot_copy(to, me).start()
        return c

    lax.fori_loop(me + 1, n_s, start_tot, 0)

    def pass_on(d, c):
        for m in range(N_PROJ):

            @pl.when(idx - 1 - d >= 0)
            def _():
                b = jnp.maximum(idx - 1 - d, 0)
                w_copy(0, b, m).wait_recv()

                @pl.when(has_right)
                def _():
                    w_copy(0, b, m).start()

            @pl.when(idx + 1 + d < n_o)
            def _():
                b = jnp.minimum(idx + 1 + d, n_o - 1)
                w_copy(1, b, m).wait_recv()

                @pl.when(has_left)
                def _():
                    w_copy(1, b, m).start()

        return c

    lax.fori_loop(0, max(n_o - 2, 0), pass_on, 0)

    def o_copy(direction, s, m, src=None):
        slot = oslot(s, m)
        b = (s // (2 * k)) * k + lax.rem(s, k)
        return remote(
            slot if src is None else src,
            slot,
            os_sem.at[direction, b, m],
            or_sem.at[direction, b, m],
            {"sp": right if direction == 0 else left},
        )

    def y_copy(b, m, arriving=False):
        s = (b // k) * (2 * k) + (1 - half if arriving else half) * k + lax.rem(b, k)
        slot = oslot(s, m)
        return remote(slot, slot, oy_sem.at[0, b, m], oy_sem.at[1, b, m], {"sp": pair})

    def start_out_own():
        for m in range(2):
            local[N_PROJ + m].wait()
            y_copy(idx, m).start()

        @pl.when(has_right)
        def _():
            for m in range(2):
                o_copy(0, me, m).start()

        @pl.when(has_left)
        def _():
            for m in range(2):
                o_copy(1, me, m).start()

    def pass_out(d, c):
        for m in range(2):

            @pl.when(idx - 1 - d >= 0)
            def _():
                b = jnp.maximum(idx - 1 - d, 0)
                o_copy(0, member(b), m).wait_recv()

                @pl.when(has_right)
                def _():
                    o_copy(0, member(b), m).start()

                y_copy(b, m).start()

            @pl.when(idx + 1 + d < n_o)
            def _():
                b = jnp.minimum(idx + 1 + d, n_o - 1)
                o_copy(1, member(b), m).wait_recv()

                @pl.when(has_left)
                def _():
                    o_copy(1, member(b), m).start()

                y_copy(b, m).start()

        return c

    start_out_own()

    cb, sb = cb_ref[me], sb_ref[me]
    lane = lax.broadcasted_iota(jnp.int32, (rows, HEAD_DIM), 1)
    cos = cj_ref[...] * cb - sj_ref[...] * sb
    sin = sj_ref[...] * cb + cj_ref[...] * sb
    sin = jnp.where(lane < HEAD_DIM // 2, -sin, sin)

    def rotate(x):
        return x * cos + pltpu.roll(x, HEAD_DIM // 2, 1) * sin

    x_copy.wait_recv()

    def p_copy(m):
        return remote(p_send.at[m], p_recv.at[m], p_sem.at[0, m], p_sem.at[1, m], {"sp": pair})

    def last_block(m):
        @pl.when(jnp.logical_and(idx - 1 - (n_o - 2) >= 0, n_o >= 2))
        def _():
            w_copy(0, 0, m).wait_recv()

        @pl.when(jnp.logical_and(idx + 1 + (n_o - 2) < n_o, n_o >= 2))
        def _():
            w_copy(1, n_o - 1, m).wait_recv()

    def multiply(m):
        local[m].wait()
        last_block(m)
        p_send[m] = dot(x_recv[...], wbuf[m]).astype(BF16)
        p_copy(m).start()
        acc[m] = dot(x_self[...], wbuf[m])

    def projected(m):
        p_copy(m).wait_recv()
        return (acc[m] + p_recv[m].astype(F32)).astype(BF16)

    def head(x, h):
        return x[:, h * HEAD_DIM : (h + 1) * HEAD_DIM]

    def st_copy(to, source):
        return remote(st_send, st_buf.at[source], ss_sem.at[to], sr_sem.at[source], {"sp": to})

    multiply(0)
    multiply(1)
    multiply(2)
    key_raw, value = projected(0), projected(1)
    qkv[1] = value
    for h in range(heads):
        at = slice(h * HEAD_DIM, (h + 1) * HEAD_DIM)
        key = rotate(head(key_raw, h).astype(F32)).astype(BF16)
        qkv[0, :, at] = key
        run = run_cols[h]
        weighted = (key.astype(F32) * jnp.exp(run[rows - 1 : rows] - run)).astype(BF16)
        st_send[at, :] = dot(weighted, head(value, h), 0, 0).astype(BF16)

    def start_state(to, c):
        st_copy(to, me).start()
        return c

    lax.fori_loop(me + 1, n_s, start_state, 0)

    multiply(3)
    gated = (
        projected(2).astype(F32) * jax.nn.sigmoid(projected(3).astype(F32))
    ).astype(BF16)
    halo_send[...] = gated[rows - HALO :]
    after = lax.rem(me + 1, n_s)
    h_copy = remote(halo_send, halo_recv, h_sem.at[0], h_sem.at[1], {"sp": after})
    h_copy.start()
    xp[HALO:, :] = gated.astype(F32)
    multiply(4)
    multiply(5)
    third = -(-(n_o - 1) // 3)
    lax.fori_loop(0, min(third, n_o - 1), pass_out, 0)

    h_copy.wait_recv()
    xp[:HALO, :] = jnp.where(me > 0, halo_recv[...].astype(F32), 0.0)
    col0 = pl.multiple_of(mt * cols, 128)
    n_taps = taps_ref.shape[0]
    taps = taps_ref[:, pl.ds(col0, cols)].astype(F32)
    total = jnp.zeros((rows, 1), F32)
    totsq = jnp.zeros((rows, 1), F32)
    for c in range(0, cols, 128):
        for r in range(0, rows, 64):
            s = jnp.zeros((64, 128), F32)
            for w in range(n_taps):
                first = r + w + HALO - (n_taps - 1)
                s = s + xp[first : first + 64, c : c + 128] * taps[w : w + 1, c : c + 128]
            csum[r : r + 64, c : c + 128] = s
    conv = csum[...]
    total = jnp.sum(conv, axis=1, keepdims=True)
    totsq = jnp.sum(conv * conv, axis=1, keepdims=True)
    diag = r_iota == c_iota
    stat_send[...] = jnp.zeros_like(stat_send)
    stat_send[0:1, :rows] = jnp.sum(jnp.where(diag, total, 0.0), axis=0, keepdims=True)
    stat_send[1:2, :rows] = jnp.sum(jnp.where(diag, totsq, 0.0), axis=0, keepdims=True)

    def stat_copy(d):
        to = lax.rem(mt + d, n_t)
        return remote(
            stat_send, stat_buf.at[d - 1], stat_sem.at[0, d - 1], stat_sem.at[1, d - 1], {"tp": to}
        )

    for d in range(1, n_t):
        stat_copy(d).start()

    lax.fori_loop(min(third, n_o - 1), min(2 * third, n_o - 1), pass_out, 0)

    query_raw = projected(4)
    for h in range(heads):
        at = slice(h * HEAD_DIM, (h + 1) * HEAD_DIM)
        query = (rotate(head(query_raw, h).astype(F32)) * HEAD_DIM ** (-0.5)).astype(BF16)
        qkv[2, :, at] = query
        weights = (dot(query, qkv[0, :, at], 1, 1) * decay[h]).astype(BF16)
        csum_h = dot(weights, qkv[1, :, at])
        acc[0, :, at] = csum_h

    state[...] = jnp.zeros_like(state)

    def carry(s, c):
        tot_copy(me, s).wait_recv()
        st_copy(me, s).wait_recv()
        for h in range(heads):
            at = slice(h * HEAD_DIM, (h + 1) * HEAD_DIM)
            factor = jnp.exp(tot_buf[s, h : h + 1, :])
            state[at, :] = state[at, :] * factor + st_buf[s, at, :].astype(F32)
        return c

    lax.fori_loop(0, me, carry, 0)
    out_gate = projected(5).astype(F32)
    gate = out_gate * jax.nn.sigmoid(out_gate)
    for h in range(heads):
        at = slice(h * HEAD_DIM, (h + 1) * HEAD_DIM)
        cross = dot(qkv[2, :, at], state[at, :].astype(BF16)) * jnp.exp(run_cols[h])
        merged = acc[0, :, at] + cross
        mean = jnp.mean(merged, axis=1, keepdims=True)
        away = merged - mean
        var = jnp.mean(away * away, axis=1, keepdims=True)
        rg = rgain_ref[:, pl.ds(pl.multiple_of(mt * cols + h * HEAD_DIM, 128), HEAD_DIM)]
        hid[1, :, at] = (gate[:, at] * (away * lax.rsqrt(var + EPSILON)) * rg).astype(BF16)

    lax.fori_loop(min(2 * third, n_o - 1), n_o - 1, pass_out, 0)

    sums = stat_send[...]
    for d in range(1, n_t):
        stat_copy(d).wait_recv()
        sums = sums + stat_buf[d - 1]
    total = jnp.sum(jnp.where(diag, sums[0:1, :rows], 0.0), axis=1, keepdims=True)
    totsq = jnp.sum(jnp.where(diag, sums[1:2, :rows], 0.0), axis=1, keepdims=True)
    mean = total / conv_dim
    var = totsq / conv_dim - mean * mean
    normed = (csum[...] - mean) * lax.rsqrt(var + EPSILON) * cgain_ref[:, pl.ds(col0, cols)]
    hid[0] = (normed * jax.nn.sigmoid(normed)).astype(BF16)

    def arrived(b, c):
        for m in range(2):
            y_copy(b, m, True).wait_recv()
        return c

    lax.fori_loop(0, n_o, arrived, 0)
    features = r_send.shape[1]
    fc = features // CHUNKS
    share = rows // n_t

    def r_copy(d, j):
        to = lax.rem(mt + d, n_t)
        at = pl.ds(j * fc, fc)
        return remote(
            r_send.at[pl.ds(pl.multiple_of(to * share, 16), share), at],
            r_buf.at[d - 1, :, at],
            rs_sem.at[0, d - 1, j],
            rs_sem.at[1, d - 1, j],
            {"tp": to},
        )

    for j in range(CHUNKS):
        at = slice(j * fc, (j + 1) * fc)
        r_send[:, at] = (
            dot(hid[0], obuf[0, at, :], 1, 1) + dot(hid[1], obuf[1, at, :], 1, 1)
        ).astype(BF16)
        for d in range(1, n_t):
            r_copy(d, j).start()

    for j in range(CHUNKS):
        at = slice(j * fc, (j + 1) * fc)
        mixed = r_send[pl.ds(pl.multiple_of(mt * share, 16), share), at].astype(F32)
        for d in range(1, n_t):
            r_copy(d, j).wait_recv()
            mixed = mixed + r_buf[d - 1, :, at].astype(F32)
        out_ref[:, at] = mixed.astype(BF16)

    x_copy.wait_send()
    h_copy.wait_send()
    for m in range(N_PROJ):
        p_copy(m).wait_send()
    for d in range(1, n_t):
        stat_copy(d).wait_send()
        for j in range(CHUNKS):
            r_copy(d, j).wait_send()

    def sent_later(to, c):
        tot_copy(to, me).wait_send()
        st_copy(to, me).wait_send()
        return c

    lax.fori_loop(me + 1, n_s, sent_later, 0)

    def sent_right(b, c):
        for m in range(N_PROJ):
            w_copy(0, b, m).wait_send()
        for m in range(2):
            o_copy(0, member(b), m).wait_send()
        return c

    def sent_left(b, c):
        for m in range(N_PROJ):
            w_copy(1, b, m).wait_send()
        for m in range(2):
            o_copy(1, member(b), m).wait_send()
        return c

    @pl.when(has_right)
    def _():
        lax.fori_loop(0, idx + 1, sent_right, 0)

    @pl.when(has_left)
    def _():
        lax.fori_loop(idx, n_o, sent_left, 0)

    def sent_pair(b, c):
        for m in range(2):
            y_copy(b, m).wait_send()
        return c

    lax.fori_loop(0, n_o, sent_pair, 0)


def tables(n_s, rows):
    freq = ROPE_BASE ** (-np.arange(0, HEAD_DIM, 2, dtype=np.float64) / HEAD_DIM)
    freq = np.concatenate([freq, freq])
    near = np.arange(rows, dtype=np.float64)[:, None] * freq
    base = (np.arange(n_s, dtype=np.float64) * rows)[:, None, None] * freq
    return [np.float32(f(a)) for a in (near, base) for f in (np.cos, np.sin)]


def solution(mesh):
    n_s, n_t = mesh.shape["sp"], mesh.shape["tp"]

    def per_device(
        tokens,
        norm_gain,
        conv_value_w,
        conv_gate_w,
        query_w,
        key_w,
        value_w,
        out_gate_w,
        conv_out_w,
        ret_out_w,
        conv_taps,
        conv_gain,
        ret_gain,
        log_decay,
    ):
        rows, d = tokens.shape
        wrows, cols = query_w.shape
        n_o = n_s // 2
        heads = cols // HEAD_DIM
        share = rows // n_t
        vmem = pl.BlockSpec(memory_space=pltpu.VMEM)
        hbm = pl.BlockSpec(memory_space=pl.ANY)
        dma = pltpu.SemaphoreType.DMA
        call = pl.pallas_call(
            functools.partial(kernel, n_s, n_t, conv_gain.shape[0]),
            out_shape=jax.ShapeDtypeStruct((share, d), BF16),
            in_specs=[hbm, vmem] + [hbm] * 8 + [vmem] * 8,
            out_specs=vmem,
            scratch_shapes=[
                pltpu.VMEM((rows, d), BF16),
                pltpu.VMEM((rows, d // 2), BF16),
                pltpu.VMEM((rows, d // 2), BF16),
                pltpu.VMEM((rows, d // 2), BF16),
                pltpu.VMEM((N_PROJ, d // 2, cols), BF16),
                pltpu.VMEM((2, d, cols), BF16),
                pltpu.VMEM((N_PROJ, rows, cols), F32),
                pltpu.VMEM((N_PROJ, rows, cols), BF16),
                pltpu.VMEM((N_PROJ, rows, cols), BF16),
                pltpu.VMEM((heads, rows, rows), F32),
                pltpu.VMEM((heads, rows, HEAD_DIM), F32),
                pltpu.VMEM((8, HEAD_DIM), F32),
                pltpu.VMEM((n_s, 8, HEAD_DIM), F32),
                pltpu.VMEM((cols, HEAD_DIM), BF16),
                pltpu.VMEM((n_s, cols, HEAD_DIM), BF16),
                pltpu.VMEM((cols, HEAD_DIM), F32),
                pltpu.VMEM((HALO, cols), BF16),
                pltpu.VMEM((HALO, cols), BF16),
                pltpu.VMEM((HALO + rows, cols), F32),
                pltpu.VMEM((rows, cols), F32),
                pltpu.VMEM((8, 256), F32),
                pltpu.VMEM((n_t - 1, 8, 256), F32),
                pltpu.VMEM((2, rows, cols), BF16),
                pltpu.VMEM((rows, d), BF16),
                pltpu.VMEM((n_t - 1, share, d), BF16),
                pltpu.VMEM((3, rows, cols), BF16),
                dma((1 + N_PROJ + 2,)),
                dma((2,)),
                dma((2, n_o, N_PROJ)),
                dma((2, n_o, N_PROJ)),
                dma((2, n_o, 2)),
                dma((2, n_o, 2)),
                dma((2, n_o, 2)),
                dma((2, N_PROJ)),
                dma((n_s,)),
                dma((n_s,)),
                dma((n_s,)),
                dma((n_s,)),
                dma((2,)),
                dma((2, n_t - 1)),
                dma((2, n_t - 1, CHUNKS)),
            ],
            compiler_params=pltpu.CompilerParams(
                collective_id=0, has_side_effects=True, vmem_limit_bytes=48 * 1024 * 1024
            ),
        )
        cj, sj, cb, sb = tables(n_s, rows)
        return call(
            tokens,
            norm_gain[None, :],
            key_w,
            value_w,
            conv_value_w,
            conv_gate_w,
            query_w,
            out_gate_w,
            conv_out_w,
            ret_out_w,
            conv_taps,
            conv_gain[None, :],
            ret_gain[None, :],
            log_decay,
            cj,
            sj,
            cb,
            sb,
        )

    return jax.shard_map(
        per_device,
        mesh=mesh,
        in_specs=(
            P("sp", None),
            P(),
            P("sp", "tp"),
            P("sp", "tp"),
            P("sp", "tp"),
            P("sp", "tp"),
            P("sp", "tp"),
            P("sp", "tp"),
            P("sp", "tp"),
            P("sp", "tp"),
            P(),
            P(),
            P(),
            P("tp", "sp"),
        ),
        out_specs=P(("sp", "tp"), None),
        check_vma=False,
    )
```

```python
import functools

import jax
import jax.numpy as jnp
import numpy as np
from jax import lax
from jax.experimental import pallas as pl
from jax.experimental.pallas import tpu as pltpu
from jax.sharding import PartitionSpec as P

HEAD_DIM = 128
EPSILON = 1e-06
ROPE_BASE = 10000.0
F32 = jnp.float32
BF16 = jnp.bfloat16
N_PROJ = 6
HALO = 32
CHUNKS = 4


def dot(a, b, ca=1, cb=0):
    return lax.dot_general(a, b, (((ca,), (cb,)), ((), ())), preferred_element_type=F32)


def kernel(
    n_s,
    n_t,
    conv_dim,
    tok_ref,
    gain_hbm,
    kw_ref,
    vw_ref,
    cvw_ref,
    cgw_ref,
    qw_ref,
    ogw_ref,
    cow_ref,
    row_ref,
    taps_hbm,
    cgain_hbm,
    rgain_hbm,
    ld_hbm,
    near_hbm,
    base_hbm,
    out_ref,
    tok,
    gain_ref,
    taps_ref,
    cgain_ref,
    rgain_ref,
    ld_ref,
    near,
    base,
    x_end,
    ret_own,
    ret_send,
    x_self,
    x_send,
    x_recv,
    wbuf,
    obuf,
    acc,
    p_send,
    p_recv,
    decay,
    run_cols,
    tot_send,
    tot_buf,
    st_send,
    st_buf,
    state,
    halo_send,
    halo_recv,
    xp,
    csum,
    stat_send,
    stat_buf,
    hid,
    r_send,
    r_buf,
    qkv,
    loc_sem,
    x_sem,
    ws_sem,
    wr_sem,
    os_sem,
    or_sem,
    oy_sem,
    p_sem,
    ts_sem,
    tr_sem,
    ss_sem,
    sr_sem,
    h_sem,
    stat_sem,
    rs_sem,
    small_sem,
    e_sem,
    q_sem,
):
    rows = tok.shape[0]
    wrows, cols = kw_ref.shape
    heads = cols // HEAD_DIM
    k = max(1, 128 // wrows)
    n_o = n_s // 2
    me = lax.axis_index("sp")
    mt = lax.axis_index("tp")
    half = lax.rem(me // k, 2)
    idx = (me // (2 * k)) * k + lax.rem(me, k)
    pair = me + k * (1 - 2 * half)

    def member(i):
        return (i // k) * (2 * k) + half * k + lax.rem(i, k)

    def remote(src, dst, ssem, rsem, where):
        return pltpu.make_async_remote_copy(
            src_ref=src,
            dst_ref=dst,
            send_sem=ssem,
            recv_sem=rsem,
            device_id=where,
            device_id_type=pl.DeviceIdType.MESH,
        )

    proj_refs = (kw_ref, vw_ref, cvw_ref, cgw_ref, qw_ref, ogw_ref)
    out_refs = (cow_ref, row_ref)

    tok_copy = pltpu.make_async_copy(tok_ref, tok, loc_sem.at[0])
    tok_copy.start()
    barrier = pltpu.get_barrier_semaphore()

    def greet_sp(d, c):
        pl.semaphore_signal(
            barrier,
            inc=1,
            device_id={"sp": lax.rem(me + d, n_s)},
            device_id_type=pl.DeviceIdType.MESH,
        )
        return c

    def greet_tp(d, c):
        pl.semaphore_signal(
            barrier,
            inc=1,
            device_id={"tp": lax.rem(mt + d, n_t)},
            device_id_type=pl.DeviceIdType.MESH,
        )
        return c

    lax.fori_loop(1, n_s, greet_sp, 0)
    lax.fori_loop(1, n_t, greet_tp, 0)

    def wslot(b, m):
        return wbuf.at[m, pl.ds(pl.multiple_of(b * wrows, wrows), wrows)]

    def oslot(s, m):
        return obuf.at[m, pl.ds(pl.multiple_of(s * wrows, wrows), wrows)]

    local = [
        pltpu.make_async_copy(r, wslot(idx, m), loc_sem.at[1 + m]) for m, r in enumerate(proj_refs)
    ] + [
        pltpu.make_async_copy(r, oslot(me, m), loc_sem.at[1 + N_PROJ + m])
        for m, r in enumerate(out_refs)
    ]
    col0 = pl.multiple_of(mt * cols, 128)
    small = [
        pltpu.make_async_copy(src, dst, small_sem.at[n])
        for n, (src, dst) in enumerate(
            (
                (gain_hbm, gain_ref),
                (ld_hbm, ld_ref),
                (taps_hbm.at[:, pl.ds(col0, cols)], taps_ref),
                (cgain_hbm.at[:, pl.ds(col0, cols)], cgain_ref),
                (rgain_hbm.at[:, pl.ds(col0, cols)], rgain_ref),
                (near_hbm, near),
                (base_hbm.at[me], base),
            )
        )
    ]
    for copy in small + local:
        copy.start()

    pl.semaphore_wait(barrier, n_s - 1 + n_t - 1)

    has_right = idx + 1 < n_o
    has_left = idx >= 1
    right = member(jnp.minimum(idx + 1, n_o - 1))
    left = member(jnp.maximum(idx - 1, 0))

    def w_copy(direction, b, m, src=None):
        slot = wslot(b, m)
        return remote(
            slot if src is None else src,
            slot,
            ws_sem.at[direction, b, m],
            wr_sem.at[direction, b, m],
            {"sp": right if direction == 0 else left},
        )

    @pl.when(has_right)
    def _():
        for m in range(N_PROJ):
            w_copy(0, idx, m, proj_refs[m]).start()

    @pl.when(has_left)
    def _():
        for m in range(N_PROJ):
            w_copy(1, idx, m, proj_refs[m]).start()

    tok_copy.wait()
    for copy in small:
        copy.wait()
    step = 256
    square = jnp.zeros((rows, 1), F32)
    for c in range(0, tok.shape[1], step):
        part = tok[:, c : c + step].astype(F32)
        square = square + jnp.sum(part * part, axis=1, keepdims=True)
    scale = lax.rsqrt(square / tok.shape[1] + EPSILON)
    width = k * wrows
    for j in range(n_s // (2 * k)):
        for side, dst in ((1 - half, x_send), (half, x_self)):
            start = pl.multiple_of((2 * j + side) * width, 128)
            part = tok[:, pl.ds(start, width)].astype(F32)
            dst[:, j * width : (j + 1) * width] = (
                part * scale * gain_ref[:, pl.ds(start, width)]
            ).astype(BF16)
    x_copy = remote(x_send, x_recv, x_sem.at[0], x_sem.at[1], {"sp": pair})
    x_copy.start()

    tot_send[...] = jnp.zeros_like(tot_send)
    r_iota = lax.broadcasted_iota(jnp.int32, (rows, rows), 0)
    c_iota = lax.broadcasted_iota(jnp.int32, (rows, rows), 1)
    for h in range(heads):
        ld = ld_ref[h : h + 1, :]
        ld_col = jnp.sum(jnp.where(r_iota == c_iota, ld, 0.0), axis=1, keepdims=True)
        run_col = jnp.sum(jnp.where(c_iota <= r_iota, ld, 0.0), axis=1, keepdims=True)
        run_row = jnp.sum(jnp.where(r_iota <= c_iota, ld_col, 0.0), axis=0, keepdims=True)
        keep = c_iota <= r_iota
        decay[h] = jnp.where(keep, jnp.exp(jnp.where(keep, run_col - run_row, 0.0)), 0.0)
        run_cols[h] = jnp.broadcast_to(run_col, (rows, HEAD_DIM))
        tot_send[h : h + 1, :] = jnp.broadcast_to(run_col[rows - 1 : rows], (1, HEAD_DIM))

    def tot_copy(to, source):
        return remote(
            tot_send, tot_buf.at[source], ts_sem.at[to], tr_sem.at[source], {"sp": to}
        )

    def start_tot(to, c):
        tot_copy(to, me).start()
        return c

    lax.fori_loop(me + 1, n_s, start_tot, 0)

    def pass_on(d, c):
        for m in range(N_PROJ):

            @pl.when(idx - 1 - d >= 0)
            def _():
                b = jnp.maximum(idx - 1 - d, 0)
                w_copy(0, b, m).wait_recv()

                @pl.when(has_right)
                def _():
                    w_copy(0, b, m).start()

            @pl.when(idx + 1 + d < n_o)
            def _():
                b = jnp.minimum(idx + 1 + d, n_o - 1)
                w_copy(1, b, m).wait_recv()

                @pl.when(has_left)
                def _():
                    w_copy(1, b, m).start()

        return c

    lax.fori_loop(0, max(n_o - 2, 0), pass_on, 0)

    def o_copy(direction, s, m, src=None):
        slot = oslot(s, m)
        b = (s // (2 * k)) * k + lax.rem(s, k)
        return remote(
            slot if src is None else src,
            slot,
            os_sem.at[direction, b, m],
            or_sem.at[direction, b, m],
            {"sp": right if direction == 0 else left},
        )

    def y_copy(b, m, arriving=False):
        s = (b // k) * (2 * k) + (1 - half if arriving else half) * k + lax.rem(b, k)
        slot = oslot(s, m)
        return remote(slot, slot, oy_sem.at[0, b, m], oy_sem.at[1, b, m], {"sp": pair})

    def start_out_own():
        for m in range(2):
            local[N_PROJ + m].wait()
            y_copy(idx, m).start()

        @pl.when(has_right)
        def _():
            for m in range(2):
                o_copy(0, me, m).start()

        @pl.when(has_left)
        def _():
            for m in range(2):
                o_copy(1, me, m).start()

    def pass_out(d, c):
        for m in range(2):

            @pl.when(idx - 1 - d >= 0)
            def _():
                b = jnp.maximum(idx - 1 - d, 0)
                o_copy(0, member(b), m).wait_recv()

                @pl.when(has_right)
                def _():
                    o_copy(0, member(b), m).start()

                y_copy(b, m).start()

            @pl.when(idx + 1 + d < n_o)
            def _():
                b = jnp.minimum(idx + 1 + d, n_o - 1)
                o_copy(1, member(b), m).wait_recv()

                @pl.when(has_left)
                def _():
                    o_copy(1, member(b), m).start()

                y_copy(b, m).start()

        return c

    start_out_own()

    cb, sb = base[0:1, :], base[1:2, :]
    lane = lax.broadcasted_iota(jnp.int32, (rows, HEAD_DIM), 1)
    cos = near[0] * cb - near[1] * sb
    sin = near[1] * cb + near[0] * sb
    sin = jnp.where(lane < HEAD_DIM // 2, -sin, sin)

    def rotate(x):
        return x * cos + pltpu.roll(x, HEAD_DIM // 2, 1) * sin

    x_copy.wait_recv()

    def p_copy(m):
        return remote(p_send.at[m], p_recv.at[m], p_sem.at[0, m], p_sem.at[1, m], {"sp": pair})

    def last_block(m):
        @pl.when(jnp.logical_and(idx - 1 - (n_o - 2) >= 0, n_o >= 2))
        def _():
            w_copy(0, 0, m).wait_recv()

        @pl.when(jnp.logical_and(idx + 1 + (n_o - 2) < n_o, n_o >= 2))
        def _():
            w_copy(1, n_o - 1, m).wait_recv()

    def multiply(m):
        local[m].wait()
        last_block(m)
        p_send[m] = dot(x_recv[...], wbuf[m]).astype(BF16)
        p_copy(m).start()
        acc[m] = dot(x_self[...], wbuf[m])

    def projected(m):
        p_copy(m).wait_recv()
        return (acc[m] + p_recv[m].astype(F32)).astype(BF16)

    def head(x, h):
        return x[:, h * HEAD_DIM : (h + 1) * HEAD_DIM]

    def st_copy(to, source):
        return remote(st_send, st_buf.at[source], ss_sem.at[to], sr_sem.at[source], {"sp": to})

    multiply(0)
    multiply(1)
    multiply(2)
    key_raw, value = projected(0), projected(1)
    qkv[1] = value
    for h in range(heads):
        at = slice(h * HEAD_DIM, (h + 1) * HEAD_DIM)
        key = rotate(head(key_raw, h).astype(F32)).astype(BF16)
        qkv[0, :, at] = key
        run = run_cols[h]
        weighted = (key.astype(F32) * jnp.exp(run[rows - 1 : rows] - run)).astype(BF16)
        st_send[at, :] = dot(weighted, head(value, h), 0, 0).astype(BF16)

    def start_state(to, c):
        st_copy(to, me).start()
        return c

    lax.fori_loop(me + 1, n_s, start_state, 0)

    multiply(3)
    gated = (
        projected(2).astype(F32) * jax.nn.sigmoid(projected(3).astype(F32))
    ).astype(BF16)
    halo_send[...] = gated[rows - HALO :]
    after = lax.rem(me + 1, n_s)
    h_copy = remote(halo_send, halo_recv, h_sem.at[0], h_sem.at[1], {"sp": after})
    h_copy.start()
    xp[HALO:, :] = gated.astype(F32)
    multiply(4)
    multiply(5)
    third = -(-(n_o - 1) // 3)
    lax.fori_loop(0, min(third, n_o - 1), pass_out, 0)

    h_copy.wait_recv()
    xp[:HALO, :] = jnp.where(me > 0, halo_recv[...].astype(F32), 0.0)
    n_taps = taps_ref.shape[0]
    taps = taps_ref[...].astype(F32)
    for c in range(0, cols, 128):
        for r in range(0, rows, 64):
            s = jnp.zeros((64, 128), F32)
            for w in range(n_taps):
                first = r + w + HALO - (n_taps - 1)
                s = s + xp[first : first + 64, c : c + 128] * taps[w : w + 1, c : c + 128]
            csum[r : r + 64, c : c + 128] = s
    conv = csum[...]
    total = jnp.sum(conv, axis=1, keepdims=True)
    totsq = jnp.sum(conv * conv, axis=1, keepdims=True)
    diag = r_iota == c_iota
    stat_send[...] = jnp.zeros_like(stat_send)
    stat_send[0:1, :rows] = jnp.sum(jnp.where(diag, total, 0.0), axis=0, keepdims=True)
    stat_send[1:2, :rows] = jnp.sum(jnp.where(diag, totsq, 0.0), axis=0, keepdims=True)

    def stat_copy(d):
        to = lax.rem(mt + d, n_t)
        return remote(
            stat_send, stat_buf.at[d - 1], stat_sem.at[0, d - 1], stat_sem.at[1, d - 1], {"tp": to}
        )

    for d in range(1, n_t):
        stat_copy(d).start()

    lax.fori_loop(min(third, n_o - 1), min(2 * third, n_o - 1), pass_out, 0)

    query_raw = projected(4)
    for h in range(heads):
        at = slice(h * HEAD_DIM, (h + 1) * HEAD_DIM)
        query = (rotate(head(query_raw, h).astype(F32)) * HEAD_DIM ** (-0.5)).astype(BF16)
        qkv[2, :, at] = query
        weights = (dot(query, qkv[0, :, at], 1, 1) * decay[h]).astype(BF16)
        csum_h = dot(weights, qkv[1, :, at])
        acc[0, :, at] = csum_h

    state[...] = jnp.zeros_like(state)

    def carry(s, c):
        tot_copy(me, s).wait_recv()
        st_copy(me, s).wait_recv()
        for h in range(heads):
            at = slice(h * HEAD_DIM, (h + 1) * HEAD_DIM)
            factor = jnp.exp(tot_buf[s, h : h + 1, :])
            state[at, :] = state[at, :] * factor + st_buf[s, at, :].astype(F32)
        return c

    lax.fori_loop(0, me, carry, 0)
    out_gate = projected(5).astype(F32)
    gate = out_gate * jax.nn.sigmoid(out_gate)
    for h in range(heads):
        at = slice(h * HEAD_DIM, (h + 1) * HEAD_DIM)
        cross = dot(qkv[2, :, at], state[at, :].astype(BF16)) * jnp.exp(run_cols[h])
        merged = acc[0, :, at] + cross
        mean = jnp.mean(merged, axis=1, keepdims=True)
        away = merged - mean
        var = jnp.mean(away * away, axis=1, keepdims=True)
        rg = rgain_ref[:, at]
        hid[1, :, at] = (gate[:, at] * (away * lax.rsqrt(var + EPSILON)) * rg).astype(BF16)

    lax.fori_loop(min(2 * third, n_o - 1), n_o - 1, pass_out, 0)

    sums = stat_send[...]
    for d in range(1, n_t):
        stat_copy(d).wait_recv()
        sums = sums + stat_buf[d - 1]
    total = jnp.sum(jnp.where(diag, sums[0:1, :rows], 0.0), axis=1, keepdims=True)
    totsq = jnp.sum(jnp.where(diag, sums[1:2, :rows], 0.0), axis=1, keepdims=True)
    mean = total / conv_dim
    var = totsq / conv_dim - mean * mean
    normed = (csum[...] - mean) * lax.rsqrt(var + EPSILON) * cgain_ref[...]
    hid[0] = (normed * jax.nn.sigmoid(normed)).astype(BF16)

    def arrived(b, c):
        for m in range(2):
            y_copy(b, m, True).wait_recv()
        return c

    lax.fori_loop(0, n_o, arrived, 0)
    features = r_send.shape[1]
    fc = features // CHUNKS
    share = rows // n_t

    def r_copy(d, j):
        to = lax.rem(mt + d, n_t)
        at = pl.ds(j * fc, fc)
        return remote(
            r_send.at[pl.ds(pl.multiple_of(to * share, 16), share), at],
            r_buf.at[d - 1, :, at],
            rs_sem.at[0, d - 1, j],
            rs_sem.at[1, d - 1, j],
            {"tp": to},
        )

    for j in range(CHUNKS):
        at = slice(j * fc, (j + 1) * fc)
        r_send[:, at] = (
            dot(hid[0], obuf[0, at, :], 1, 1) + dot(hid[1], obuf[1, at, :], 1, 1)
        ).astype(BF16)
        for d in range(1, n_t):
            r_copy(d, j).start()

    for j in range(CHUNKS):
        at = slice(j * fc, (j + 1) * fc)
        mixed = r_send[pl.ds(pl.multiple_of(mt * share, 16), share), at].astype(F32)
        for d in range(1, n_t):
            r_copy(d, j).wait_recv()
            mixed = mixed + r_buf[d - 1, :, at].astype(F32)
        out_ref[:, at] = mixed.astype(BF16)

    x_copy.wait_send()
    h_copy.wait_send()
    for m in range(N_PROJ):
        p_copy(m).wait_send()
    for d in range(1, n_t):
        stat_copy(d).wait_send()
        for j in range(CHUNKS):
            r_copy(d, j).wait_send()

    def sent_later(to, c):
        tot_copy(to, me).wait_send()
        st_copy(to, me).wait_send()
        return c

    lax.fori_loop(me + 1, n_s, sent_later, 0)

    def sent_right(b, c):
        for m in range(N_PROJ):
            w_copy(0, b, m).wait_send()
        for m in range(2):
            o_copy(0, member(b), m).wait_send()
        return c

    def sent_left(b, c):
        for m in range(N_PROJ):
            w_copy(1, b, m).wait_send()
        for m in range(2):
            o_copy(1, member(b), m).wait_send()
        return c

    @pl.when(has_right)
    def _():
        lax.fori_loop(0, idx + 1, sent_right, 0)

    @pl.when(has_left)
    def _():
        lax.fori_loop(idx, n_o, sent_left, 0)

    def sent_pair(b, c):
        for m in range(2):
            y_copy(b, m).wait_send()
        return c

    lax.fori_loop(0, n_o, sent_pair, 0)


def tables(n_s, rows):
    freq = ROPE_BASE ** (-np.arange(0, HEAD_DIM, 2, dtype=np.float64) / HEAD_DIM)
    freq = np.concatenate([freq, freq])
    near = np.arange(rows, dtype=np.float64)[:, None] * freq
    base = (np.arange(n_s, dtype=np.float64) * rows)[:, None, None] * freq
    near = np.stack([np.cos(near), np.sin(near)])
    base = np.concatenate([np.cos(base), np.sin(base), np.zeros((n_s, 6, HEAD_DIM))], axis=1)
    return np.float32(near), np.float32(base)


def solution(mesh):
    n_s, n_t = mesh.shape["sp"], mesh.shape["tp"]

    def per_device(
        tokens,
        norm_gain,
        conv_value_w,
        conv_gate_w,
        query_w,
        key_w,
        value_w,
        out_gate_w,
        conv_out_w,
        ret_out_w,
        conv_taps,
        conv_gain,
        ret_gain,
        log_decay,
    ):
        rows, d = tokens.shape
        wrows, cols = query_w.shape
        n_o = n_s // 2
        heads = cols // HEAD_DIM
        share = rows // n_t
        vmem = pl.BlockSpec(memory_space=pltpu.VMEM)
        hbm = pl.BlockSpec(memory_space=pl.ANY)
        dma = pltpu.SemaphoreType.DMA
        call = pl.pallas_call(
            functools.partial(kernel, n_s, n_t, conv_gain.shape[0]),
            out_shape=jax.ShapeDtypeStruct((share, d), BF16),
            in_specs=[hbm] * 16,
            out_specs=vmem,
            scratch_shapes=[
                pltpu.VMEM((rows, d), BF16),
                pltpu.VMEM((1, d), F32),
                pltpu.VMEM((conv_taps.shape[0], cols), BF16),
                pltpu.VMEM((1, cols), F32),
                pltpu.VMEM((1, cols), F32),
                pltpu.VMEM(log_decay.shape, F32),
                pltpu.VMEM((2, rows, HEAD_DIM), F32),
                pltpu.VMEM((8, HEAD_DIM), F32),
                pltpu.VMEM((2, rows, d // 2), BF16),
                pltpu.VMEM((N_PROJ, rows, cols), BF16),
                pltpu.VMEM((2, N_PROJ, rows, cols), BF16),
                pltpu.VMEM((rows, d // 2), BF16),
                pltpu.VMEM((rows, d // 2), BF16),
                pltpu.VMEM((rows, d // 2), BF16),
                pltpu.VMEM((N_PROJ, d // 2, cols), BF16),
                pltpu.VMEM((2, d, cols), BF16),
                pltpu.VMEM((N_PROJ, rows, cols), F32),
                pltpu.VMEM((N_PROJ, rows, cols), BF16),
                pltpu.VMEM((N_PROJ, rows, cols), BF16),
                pltpu.VMEM((heads, rows, rows), F32),
                pltpu.VMEM((heads, rows, HEAD_DIM), F32),
                pltpu.VMEM((8, HEAD_DIM), F32),
                pltpu.VMEM((n_s, 8, HEAD_DIM), F32),
                pltpu.VMEM((cols, HEAD_DIM), BF16),
                pltpu.VMEM((n_s, cols, HEAD_DIM), BF16),
                pltpu.VMEM((cols, HEAD_DIM), F32),
                pltpu.VMEM((HALO, cols), BF16),
                pltpu.VMEM((HALO, cols), BF16),
                pltpu.VMEM((HALO + rows, cols), F32),
                pltpu.VMEM((rows, cols), F32),
                pltpu.VMEM((8, 256), F32),
                pltpu.VMEM((n_t - 1, 8, 256), F32),
                pltpu.VMEM((2, rows, cols), BF16),
                pltpu.VMEM((rows, d), BF16),
                pltpu.VMEM((n_t - 1, share, d), BF16),
                pltpu.VMEM((3, rows, cols), BF16),
                dma((1 + N_PROJ + 2,)),
                dma((2,)),
                dma((2, n_o, N_PROJ)),
                dma((2, n_o, N_PROJ)),
                dma((2, n_o, 2)),
                dma((2, n_o, 2)),
                dma((2, n_o, 2)),
                dma((2, N_PROJ)),
                dma((n_s,)),
                dma((n_s,)),
                dma((n_s,)),
                dma((n_s,)),
                dma((2,)),
                dma((2, n_t - 1)),
                dma((2, n_t - 1, CHUNKS)),
                dma((7,)),
                dma((2, 2)),
                dma((2, 2, N_PROJ)),
            ],
            compiler_params=pltpu.CompilerParams(
                collective_id=0, has_side_effects=True, vmem_limit_bytes=67043328
            ),
        )
        near, base = tables(n_s, rows)
        return call(
            tokens,
            norm_gain[None, :],
            key_w,
            value_w,
            conv_value_w,
            conv_gate_w,
            query_w,
            out_gate_w,
            conv_out_w,
            ret_out_w,
            conv_taps,
            conv_gain[None, :],
            ret_gain[None, :],
            log_decay,
            near,
            base,
        )

    return jax.shard_map(
        per_device,
        mesh=mesh,
        in_specs=(
            P("sp", None),
            P(),
            P("sp", "tp"),
            P("sp", "tp"),
            P("sp", "tp"),
            P("sp", "tp"),
            P("sp", "tp"),
            P("sp", "tp"),
            P("sp", "tp"),
            P("sp", "tp"),
            P(),
            P(),
            P(),
            P("tp", "sp"),
        ),
        out_specs=P(("sp", "tp"), None),
        check_vma=False,
    )
```
